32 devices in a mesh: rep: 2 (over x), fs: 4 (over y, core), tp: 4 (over z).
Axes of the slice: x: 2, y: 2, z: 4, core: 2. Of those that a mesh axis runs over, the one named last changes fastest.
Arguments:
- tokens: bfloat16 [4096, 2048], P(('rep', 'fs', 'tp')), may hold values from -3 to 3
- mixer_output: bfloat16 [4096, 2048], P(('rep', 'fs', 'tp')), may hold values from -6 to 6
- early_norm: float32 [2048], replicated, may hold values from 0.75 to 1.25
- early_gate: bfloat16 [2048, 5120], P('fs', 'tp'), may hold values from -0.125 to 0.125
- early_value: bfloat16 [2048, 5120], P('fs', 'tp'), may hold values from -0.125 to 0.125
- early_down: bfloat16 [5120, 2048], P('tp', 'fs'), may hold values from -0.078125 to 0.078125
- early_post: float32 [2048], replicated, may hold values from 0.75 to 1.25
- mixer_gain: float32 [2048], replicated, may hold values from 0.75 to 1.25
- later_norm: float32 [2048], replicated, may hold values from 0.75 to 1.25
- later_gate: bfloat16 [2048, 5120], P('fs', 'tp'), may hold values from -0.125 to 0.125
- later_value: bfloat16 [2048, 5120], P('fs', 'tp'), may hold values from -0.125 to 0.125
- later_down: bfloat16 [5120, 2048], P('tp', 'fs'), may hold values from -0.078125 to 0.078125
- later_post: float32 [2048], replicated, may hold values from 0.75 to 1.25
Outputs:
- layer_out: bfloat16 [4096, 2048], P(('rep', 'fs', 'tp'))
The draws below stay inside these ranges and needn't reach their ends.
All inputs are finite; a program needn't handle non-finite values.
Results may differ from the reference program's by a relative error of at most 0.015.
Values may be sent and summed in bfloat16 or wider, within the bound.
A program may use at most 128 MiB of HBM per device.

```python
import jax
import jax.numpy as jnp
from jax import lax

D = 2048
FF = 5120
TOKENS = 4096


def steps_of(rng, extent, split, low, top_value):
    def one(position, parts):
        draws = jax.random.uniform(jax.random.fold_in(jax.random.fold_in(rng, 6), position), (parts,), jnp.float32, low / len(split), top_value / len(split))
        return jnp.repeat(jnp.exp(draws), extent[position] // parts).reshape((-1,) + (1,) * (len(extent) - position - 1))

    loudness = one(*split[0])
    for cut in split[1:]:
        loudness = loudness * one(*cut)
    return loudness


def scatter_about(stream_key, dims, scale, bound, cuts=(), dtype=jnp.bfloat16):
    array = jax.random.normal(stream_key, dims, jnp.float32) * scale
    if len(cuts) > 0:
        array = steps_of(stream_key, dims, cuts, -0.22, 0.18) * array
    return jnp.clip(array, min=-bound, max=bound).astype(dtype)


def setup_inputs(seed: int = 0) -> dict:
    keys = jax.random.split(jax.random.key(seed), 14)
    return {
        "tokens": scatter_about(keys[0], (TOKENS, D), 0.5, 3.0, ((0, 32),)),
        "mixer_output": scatter_about(keys[1], (TOKENS, D), 1.0, 6.0, ((0, 32),)),
        "early_norm": jnp.clip(1.0 + 0.05 * jax.random.normal(keys[2], (D,), jnp.float32), 0.75, 1.25),
        "early_gate": scatter_about(keys[3], (D, FF), D ** -0.5, 0.125, ((0, 4), (1, 4))),
        "early_value": scatter_about(keys[4], (D, FF), D ** -0.5, 0.125, ((0, 4), (1, 4))),
        "early_down": scatter_about(keys[5], (FF, D), FF ** -0.5, 0.078125, ((0, 4), (1, 4))),
        "early_post": jnp.clip(1.0 + 0.05 * jax.random.normal(keys[6], (D,), jnp.float32), 0.75, 1.25),
        "mixer_gain": jnp.clip(1.0 + 0.05 * jax.random.normal(keys[7], (D,), jnp.float32), 0.75, 1.25),
        "later_norm": jnp.clip(1.0 + 0.05 * jax.random.normal(keys[8], (D,), jnp.float32), 0.75, 1.25),
        "later_gate": scatter_about(keys[9], (D, FF), D ** -0.5, 0.125, ((0, 4), (1, 4))),
        "later_value": scatter_about(keys[10], (D, FF), D ** -0.5, 0.125, ((0, 4), (1, 4))),
        "later_down": scatter_about(keys[11], (FF, D), FF ** -0.5, 0.078125, ((0, 4), (1, 4))),
        "later_post": jnp.clip(1.0 + 0.05 * jax.random.normal(keys[12], (D,), jnp.float32), 0.75, 1.25),
    }


epsilon = 1e-06

def rms_scale(values, gain):
    values = values.astype(jnp.float32)
    scale = lax.rsqrt(lax.optimization_barrier(jnp.mean(values * values, axis=-1, keepdims=True)) + epsilon)
    return values * scale * gain

def half_branch(normed, w_gate, w_value, w_down):
    gate_sum = jnp.dot(normed, w_gate, preferred_element_type=jnp.float32)
    value_sum = jnp.dot(normed, w_value, preferred_element_type=jnp.float32)
    hidden = (jax.nn.silu(gate_sum) * value_sum).astype(jnp.bfloat16)
    return jnp.dot(hidden, w_down, preferred_element_type=jnp.float32)

def reference(tokens, mixer_output, early_norm, early_gate, early_value, early_down, early_post, mixer_gain, later_norm, later_gate, later_value, later_down, later_post):
    early_in = rms_scale(tokens, early_norm).astype(jnp.bfloat16)
    early_branch = half_branch(early_in, early_gate, early_value, early_down)
    mixed = tokens.astype(jnp.float32) + 0.5 * rms_scale(early_branch, early_post) + rms_scale(mixer_output, mixer_gain)
    mixed = mixed.astype(jnp.bfloat16)
    later_in = rms_scale(mixed, later_norm).astype(jnp.bfloat16)
    later_branch = half_branch(later_in, later_gate, later_value, later_down)
    layer_out = mixed.astype(jnp.float32) + 0.5 * rms_scale(later_branch, later_post)
    return layer_out.astype(jnp.bfloat16)
```

```python
import functools

import jax
import jax.numpy as jnp
from jax import lax
from jax.experimental import pallas as pl
from jax.experimental.pallas import tpu as pltpu
from jax.sharding import PartitionSpec as P

epsilon = 1e-06
CORES = 2


def rms_scale(values, gain):
    scale = lax.rsqrt(jnp.mean(values * values, axis=-1, keepdims=True) + epsilon)
    return values * scale * gain


def kernel(
    R, F, T,
    tokens, mixer, early_norm, w0, w1, w2, early_post, mixer_gain, later_norm, w3, w4, w5, later_post,
    out,
    g0, g1, g2, g3, g4, g5, rows0, rows1, hidden, part, mixed, from_left, from_right,
    w_send, w_recv, local_sem, z_send, z_recv,
):
    source = (w0, w1, w2, w3, w4, w5)
    full = (g0, g1, g2, g3, g4, g5)
    all_rows = (rows0, rows1)
    r, f, t = lax.axis_index("rep"), lax.axis_index("fs"), lax.axis_index("tp")
    G = F // CORES
    g, c = f // CORES, f % CORES
    n, D = tokens.shape
    half = T // 2
    cut = D // 2
    mate = {"fs": g * CORES + 1 - c}
    ahead = {"fs": (g + 1) % G * CORES + c}
    behind = {"fs": (g + G - 1) % G * CORES + c}
    z_right, z_left = {"tp": (t + 1) % T}, {"tp": (t + T - 1) % T}
    peers = [{"rep": (r + k) % R} for k in range(1, R)]

    partners = [mate] + peers
    if G > 1:
        partners += [ahead] if G == 2 else [ahead, behind]
    partners += [z_right] if T == 2 else [z_right, z_left]
    barrier = pltpu.get_barrier_semaphore()
    for who in partners:
        pl.semaphore_signal(barrier, inc=1, device_id=who, device_id_type=pl.DeviceIdType.MESH)
    pl.semaphore_wait(barrier, len(partners))

    pending, done = [], set()

    def send(src, dst, sems, index, who):
        copy = pltpu.make_async_remote_copy(
            src_ref=src, dst_ref=dst, send_sem=sems[0].at[index], recv_sem=sems[1].at[index],
            device_id=who, device_id_type=pl.DeviceIdType.MESH,
        )
        copy.start()
        pending.append(copy)
        return copy

    slots = {}

    def w_index(*key):
        return slots.setdefault(key, len(slots))

    copies = {}

    def piece(m, shard, q):
        if m % 3 == 2:
            count = full[m].shape[1] // R
            return full[m].at[shard, pl.ds(pl.multiple_of(q * count, count), count)]
        depth = source[m].shape[0]
        count = depth // R
        return full[m].at[pl.ds(pl.multiple_of(shard * depth + q * count, count), count)]

    def whole_shard(m, shard):
        if m % 3 == 2:
            return full[m].at[shard]
        depth = source[m].shape[0]
        return full[m].at[pl.ds(pl.multiple_of(shard * depth, depth), depth)]

    W = (w_send, w_recv)

    def w_send_to(key, src, dst, who):
        copies[key] = send(src, dst, W, w_index(*key), who)

    def start_weights(m):
        if G > 1:
            count = source[m].shape[0] // R
            own = source[m].at[pl.ds(pl.multiple_of(r * count, count), count)]
            w_send_to(("ring", m, 1), own, piece(m, f, r), ahead)
        w_send_to(("own", m), source[m], whole_shard(m, f), mate)
        local = pltpu.make_async_copy(source[m], whole_shard(m, f), local_sem.at[m])
        local.start()
        copies["local", m] = local

    def ring_relay(m):
        for s in range(1, G):
            copies["ring", m, s].wait_recv()
            got = piece(m, (g + G - s) % G * CORES + c, r)
            if s < G - 1:
                w_send_to(("ring", m, s + 1), got, got, ahead)
            for k, who in enumerate(peers):
                w_send_to(("peer", m, s, k), got, got, who)
            w_send_to(("mate", m, s), got, got, mate)

    def peer_relay(m):
        for s in range(1, G):
            for k in range(len(peers)):
                copies["peer", m, s, k].wait_recv()
                got = piece(m, (g + G - s) % G * CORES + c, (r + R - 1 - k) % R)
                w_send_to(("pass", m, s, k), got, got, mate)

    def ready(m):
        copies["local", m].wait()
        copies["own", m].wait_recv()
        for s in range(1, G):
            copies["mate", m, s].wait_recv()
            for k in range(len(peers)):
                copies["pass", m, s, k].wait_recv()

    Z = (z_send, z_recv)

    def block(where, ref):
        return ref.at[pl.ds(pl.multiple_of(where * n, n), n)]

    def sides(ref, d):
        return (ref.at[:, :cut], ref.at[:, cut:]) if d == half else (ref, ref)

    def z_slot(phase, layer, step, way):
        return ((phase * 2 + layer) * half + step) * 2 + way

    def gather_send(layer, d):
        rows = all_rows[layer]
        a = sides(block((t + T - (d - 1)) % T, rows), d)[0]
        b = sides(block((t + d - 1) % T, rows), d)[1]
        copies["ag", layer, d] = (
            send(a, a, Z, z_slot(0, layer, d - 1, 0), z_right),
            send(b, b, Z, z_slot(0, layer, d - 1, 1), z_left),
        )

    def gather_wait(layer, d):
        for copy in copies["ag", layer, d]:
            copy.wait_recv()

    def sum_send(layer, k):
        d = half - k
        a = sides(block((t + d) % T, part), d)[0]
        b = sides(block((t + T - d) % T, part), d)[1]
        to_a = sides(from_left.at[layer * half + k], d)[0]
        to_b = sides(from_right.at[layer * half + k], d)[1]
        copies["rs", layer, k] = (
            send(a, to_a, Z, z_slot(1, layer, k, 0), z_right),
            send(b, to_b, Z, z_slot(1, layer, k, 1), z_left),
        )

    def sum_step(layer, k):
        for copy in copies["rs", layer, k - 1]:
            copy.wait_recv()
        d = half - k
        for way, where, buffer in ((0, (t + d) % T, from_left), (1, (t + T - d) % T, from_right)):
            mine = sides(block(where, part), d + 1)[way]
            came = sides(buffer.at[layer * half + k - 1], d + 1)[way]
            mine[...] = (mine[...].astype(jnp.float32) + came[...].astype(jnp.float32)).astype(jnp.bfloat16)
        sum_send(layer, k)

    def sum_own(layer):
        for copy in copies["rs", layer, half - 1]:
            copy.wait_recv()
        own = block(t, part)[...].astype(jnp.float32)
        a = from_left.at[layer * half + half - 1]
        b = from_right.at[layer * half + half - 1]
        if half > 1:
            return own + a[...].astype(jnp.float32) + b[...].astype(jnp.float32)
        came = jnp.concatenate([a[:, :cut], b[:, cut:]], axis=1)
        return own + came.astype(jnp.float32)

    def up(layer):
        gate, value = full[3 * layer], full[3 * layer + 1]
        wide = gate.shape[1]
        tile = 256 if wide % 256 == 0 else 128

        @pl.loop(0, wide // tile)
        def _(j):
            at = pl.ds(pl.multiple_of(j * tile, tile), tile)
            x = all_rows[layer][...]
            a = jnp.dot(x, gate[:, at], preferred_element_type=jnp.float32)
            b = jnp.dot(x, value[:, at], preferred_element_type=jnp.float32)
            hidden[:, at] = (a / (1.0 + jnp.exp(-a)) * b).astype(jnp.bfloat16)

    def down(layer):
        weight = full[3 * layer + 2]
        wide = weight.shape[2]
        tile = 256 if wide % 256 == 0 else 128
        per = wide // tile

        @pl.loop(0, F * per)
        def _(j):
            inside = pl.ds(pl.multiple_of(j % per * tile, tile), tile)
            at = pl.ds(pl.multiple_of(j * tile, tile), tile)
            y = jnp.dot(hidden[...], weight[j // per, :, inside], preferred_element_type=jnp.float32)
            part[:, at] = y.astype(jnp.bfloat16)

    start_weights(0)
    start_weights(1)
    block(t, rows0)[...] = rms_scale(tokens[...].astype(jnp.float32), early_norm[...]).astype(jnp.bfloat16)
    gather_send(0, 1)
    for m in range(2, 6):
        start_weights(m)
    ring_relay(0)
    for d in range(1, half):
        gather_wait(0, d)
        gather_send(0, d + 1)
    ring_relay(1)
    peer_relay(0)
    gather_wait(0, half)
    ring_relay(2)
    peer_relay(1)
    ready(0)
    ready(1)
    up(0)
    ring_relay(3)
    peer_relay(2)
    ready(2)
    down(0)
    sum_send(0, 0)
    for k in range(1, half):
        sum_step(0, k)
    ring_relay(4)
    peer_relay(3)
    branch = sum_own(0)
    keep = (
        tokens[...].astype(jnp.float32)
        + 0.5 * rms_scale(branch, early_post[...])
        + rms_scale(mixer[...].astype(jnp.float32), mixer_gain[...])
    ).astype(jnp.bfloat16)
    mixed[...] = keep
    block(t, rows1)[...] = rms_scale(keep.astype(jnp.float32), later_norm[...]).astype(jnp.bfloat16)
    gather_send(1, 1)
    for k in range(half):
        for copy in copies["rs", 0, k]:
            copy.wait_send()
            done.add(id(copy))
    ring_relay(5)
    peer_relay(4)
    for d in range(1, half):
        gather_wait(1, d)
        gather_send(1, d + 1)
    gather_wait(1, half)
    ready(3)
    ready(4)
    up(1)
    peer_relay(5)
    ready(5)
    down(1)
    sum_send(1, 0)
    for k in range(1, half):
        sum_step(1, k)
    branch = sum_own(1)
    out[...] = (
        mixed[...].astype(jnp.float32) + 0.5 * rms_scale(branch, later_post[...])
    ).astype(jnp.bfloat16)
    for copy in pending:
        if id(copy) not in done:
            copy.wait_send()


def on_device(sizes, *args):
    R, F, T = sizes
    (tokens, mixer, early_norm, eg, ev, ed, early_post, mixer_gain, later_norm, lg, lv, ld, later_post) = args
    n, D = tokens.shape
    depth, wide = eg.shape
    bf16 = jnp.bfloat16
    gains = [x.reshape(1, D) for x in (early_norm, early_post, mixer_gain, later_norm, later_post)]
    vmem = pl.BlockSpec(memory_space=pltpu.VMEM)
    hbm = pl.BlockSpec(memory_space=pl.ANY)
    gathered = [pltpu.VMEM((F * depth, wide), bf16)] * 2 + [pltpu.VMEM((F,) + ed.shape, bf16)]
    G = F // CORES
    w_count = 6 * (1 + (G - 1) * 2 * R)
    z_count = 4 * T
    return pl.pallas_call(
        functools.partial(kernel, R, F, T),
        out_shape=jax.ShapeDtypeStruct((n, D), bf16),
        in_specs=[vmem] * 3 + [hbm] * 3 + [vmem] * 3 + [hbm] * 3 + [vmem],
        out_specs=vmem,
        scratch_shapes=gathered * 2
        + [
            pltpu.VMEM((T * n, D), bf16),
            pltpu.VMEM((T * n, D), bf16),
            pltpu.VMEM((T * n, wide), bf16),
            pltpu.VMEM((T * n, D), bf16),
            pltpu.VMEM((n, D), bf16),
            pltpu.VMEM((T, n, D), bf16),
            pltpu.VMEM((T, n, D), bf16),
            pltpu.SemaphoreType.DMA((w_count,)),
            pltpu.SemaphoreType.DMA((w_count,)),
            pltpu.SemaphoreType.DMA((6,)),
            pltpu.SemaphoreType.DMA((z_count,)),
            pltpu.SemaphoreType.DMA((z_count,)),
        ],
        compiler_params=pltpu.CompilerParams(
            collective_id=0, has_side_effects=True, vmem_limit_bytes=66_000_000
        ),
    )(tokens, mixer, gains[0], eg, ev, ed, gains[1], gains[2], gains[3], lg, lv, ld, gains[4])


def solution(mesh):
    placed = (
        P(("rep", "fs", "tp"), None),
        P(("rep", "fs", "tp"), None),
        P(),
        P("fs", "tp"),
        P("fs", "tp"),
        P("tp", "fs"),
        P(),
        P(),
        P(),
        P("fs", "tp"),
        P("fs", "tp"),
        P("tp", "fs"),
        P(),
    )
    sizes = tuple(mesh.shape[name] for name in ("rep", "fs", "tp"))
    return jax.shard_map(
        functools.partial(on_device, sizes),
        mesh=mesh,
        in_specs=placed,
        out_specs=P(("rep", "fs", "tp"), None),
        check_vma=False,
    )
```

```python
import functools

import jax
import jax.numpy as jnp
from jax import lax
from jax.experimental import pallas as pl
from jax.experimental.pallas import tpu as pltpu
from jax.sharding import PartitionSpec as P

epsilon = 1e-06
CORES = 2


def rms_scale(values, gain):
    scale = lax.rsqrt(jnp.mean(values * values, axis=-1, keepdims=True) + epsilon)
    return values * scale * gain


def kernel(
    R, F, T, B,
    tokens, mixer, early_norm, w0, w1, w2, early_post, mixer_gain, later_norm, w3, w4, w5, later_post,
    out,
    g0, g1, g2, g3, g4, g5, rows0, rows1, hidden, part0, part1, mixed, from_left, from_right, total,
    w_send, w_recv, local_sem, z_send, z_recv,
):
    source = (w0, w1, w2, w3, w4, w5)
    full = (g0, g1, g2, g3, g4, g5)
    all_rows, parts = (rows0, rows1), (part0, part1)
    r, f, t = lax.axis_index("rep"), lax.axis_index("fs"), lax.axis_index("tp")
    G = F // CORES
    g, c = f // CORES, f % CORES
    U = max(1, 4 // G)
    n, D = tokens.shape
    nb = n // B
    mate = {"fs": g * CORES + 1 - c}
    ahead = {"fs": (g + 1) % G * CORES + c}
    behind = {"fs": (g + G - 1) % G * CORES + c}
    z_right, z_left = {"tp": (t + 1) % T}, {"tp": (t + T - 1) % T}
    peers = [{"rep": (r + k) % R} for k in range(1, R)]

    partners = [mate] + peers
    if G > 1:
        partners += [ahead] if G == 2 else [ahead, behind]
    partners += [z_right] if T == 2 else [z_right, z_left]
    barrier = pltpu.get_barrier_semaphore()
    for who in partners:
        pl.semaphore_signal(barrier, inc=1, device_id=who, device_id_type=pl.DeviceIdType.MESH)
    pl.semaphore_wait(barrier, len(partners))

    pending = []

    def send(src, dst, sems, index, who):
        copy = pltpu.make_async_remote_copy(
            src_ref=src, dst_ref=dst, send_sem=sems[0].at[index], recv_sem=sems[1].at[index],
            device_id=who, device_id_type=pl.DeviceIdType.MESH,
        )
        copy.start()
        pending.append(copy)
        return copy

    slots = {}

    def w_index(*key):
        return slots.setdefault(key, len(slots))

    copies = {}

    def piece(m, shard, q, u):
        q = q * U + u
        if m % 3 == 2:
            count = full[m].shape[1] // (R * U)
            return full[m].at[shard, pl.ds(pl.multiple_of(q * count, count), count)]
        depth = source[m].shape[0]
        count = depth // (R * U)
        return full[m].at[pl.ds(pl.multiple_of(shard * depth + q * count, count), count)]

    def whole_shard(m, shard):
        if m % 3 == 2:
            return full[m].at[shard]
        depth = source[m].shape[0]
        return full[m].at[pl.ds(pl.multiple_of(shard * depth, depth), depth)]

    W = (w_send, w_recv)

    def w_send_to(key, src, dst, who):
        copies[key] = send(src, dst, W, w_index(*key), who)

    def start_weights(m):
        if G > 1:
            count = source[m].shape[0] // (R * U)
            for u in range(U):
                own = source[m].at[pl.ds(pl.multiple_of((r * U + u) * count, count), count)]
                w_send_to(("ring", m, u, 1), own, piece(m, f, r, u), ahead)
        w_send_to(("own", m), source[m], whole_shard(m, f), mate)
        local = pltpu.make_async_copy(source[m], whole_shard(m, f), local_sem.at[m])
        local.start()
        copies["local", m] = local

    def ring_relay(m, u):
        for s in range(1, G):
            copies["ring", m, u, s].wait_recv()
            got = piece(m, (g + G - s) % G * CORES + c, r, u)
            if s < G - 1:
                w_send_to(("ring", m, u, s + 1), got, got, ahead)
            for k, who in enumerate(peers):
                w_send_to(("peer", m, u, s, k), got, got, who)
            w_send_to(("mate", m, u, s), got, got, mate)

    def peer_relay(m, u):
        for s in range(1, G):
            for k in range(len(peers)):
                copies["peer", m, u, s, k].wait_recv()
                got = piece(m, (g + G - s) % G * CORES + c, (r + R - 1 - k) % R, u)
                w_send_to(("pass", m, u, s, k), got, got, mate)

    todo = [("y", 0, u) for u in range(min(1, U))]
    for i in range(1, 6 * U):
        todo += [("y", i // U, i % U), ("x", (i - 1) // U, (i - 1) % U)]
    todo.append(("x", 5, U - 1))

    def relay(upto):
        while todo and upto in todo:
            kind, m, u = todo.pop(0)
            (ring_relay if kind == "y" else peer_relay)(m, u)

    def ready(m):
        copies["local", m].wait()
        copies["own", m].wait_recv()
        for u in range(U):
            for s in range(1, G):
                copies["mate", m, u, s].wait_recv()
                for k in range(len(peers)):
                    copies["pass", m, u, s, k].wait_recv()

    sent = []

    def z_copy(src, dst, kind, layer, b, step, way):
        index = (((kind * 2 + layer) * B + b) * T + step) * 2 + way
        return pltpu.make_async_remote_copy(
            src_ref=src, dst_ref=dst, send_sem=z_send.at[index], recv_sem=z_recv.at[index],
            device_id=(z_right, z_left)[way], device_id_type=pl.DeviceIdType.MESH,
        )

    def z_start(when, copy):
        pl.when(when)(copy.start)
        sent.append((when, copy))

    def batch(b, where):
        return pl.ds(pl.multiple_of((b * T + where) * nb, nb), nb)

    def own_rows(b):
        return pl.ds(b * nb, nb)

    def gather_copy(layer, b, d, way):
        where = (t + T - (d - 1)) % T if way == 0 else (t + d - 1) % T
        rows = all_rows[layer].at[batch(b, where)]
        return z_copy(rows, rows, 0, layer, b, d, way)

    def gather_send(layer, b, d):
        z_start((t >= d - 1) & (t < T - 1), gather_copy(layer, b, d, 0))
        z_start((T - 1 - t >= d - 1) & (t > 0), gather_copy(layer, b, d, 1))

    def gather_wait(layer, b, d):
        pl.when(t >= d)(gather_copy(layer, b, d, 0).wait_recv)
        pl.when(T - 1 - t >= d)(gather_copy(layer, b, d, 1).wait_recv)

    def gather_step(layer, b, d):
        gather_wait(layer, b, d)
        if d < T - 1:
            gather_send(layer, b, d + 1)

    def came(layer, b, where, way):
        return (from_left, from_right)[way].at[(layer * B + b) * T + where]

    def sum_copy(layer, b, where, way):
        return z_copy(parts[layer].at[batch(b, where)], came(layer, b, where, way), 1, layer, b, where, way)

    def sum_first(layer, b):
        for i in range(T - 1):
            for way, where in ((0, T - 1 - i), (1, i)):
                z_start(t == (0, T - 1)[way], sum_copy(layer, b, where, way))

    def sum_step(layer, b, i):
        low = t < T // 2
        for way, where, side in ((0, T - 1 - i, low), (1, i, t >= 0), (0, T - 1 - i, ~low)):
            copy = sum_copy(layer, b, where, way)
            middle = side & ((t > 0) & (t < where) if way == 0 else (t < T - 1) & (t > where))
            last = side & (t == where) & ((t > 0) if way == 0 else (t < T - 1))

            @pl.when(middle)
            def _():
                copy.wait_recv()
                mine = parts[layer].at[batch(b, where)]
                mine[...] = (
                    mine[...].astype(jnp.float32) + came(layer, b, where, way)[...].astype(jnp.float32)
                ).astype(jnp.bfloat16)
                copy.start()

            sent.append((middle, copy))
            pl.when(last)(copy.wait_recv)

    def sum_own(layer, b):
        total[...] = parts[layer][batch(b, t)].astype(jnp.float32)
        for way, here in ((0, t > 0), (1, t < T - 1)):

            @pl.when(here)
            def _():
                total[...] += came(layer, b, t, way)[...].astype(jnp.float32)

        return total[...]

    def up(layer, b):
        gate, value = full[3 * layer], full[3 * layer + 1]
        wide = gate.shape[1]
        tile = 256 if wide % 256 == 0 else 128
        rows = pl.ds(b * T * nb, T * nb)

        @pl.loop(0, wide // tile)
        def _(j):
            at = pl.ds(pl.multiple_of(j * tile, tile), tile)
            x = all_rows[layer][rows]
            p = jnp.dot(x, gate[:, at], preferred_element_type=jnp.float32)
            v = jnp.dot(x, value[:, at], preferred_element_type=jnp.float32)
            hidden[rows, at] = (p / (1.0 + jnp.exp(-p)) * v).astype(jnp.bfloat16)

    def down(layer, b):
        weight = full[3 * layer + 2]
        wide = weight.shape[2]
        tile = 256 if wide % 256 == 0 else 128
        per = wide // tile
        rows = pl.ds(b * T * nb, T * nb)

        @pl.loop(0, F * per)
        def _(j):
            inside = pl.ds(pl.multiple_of(j % per * tile, tile), tile)
            at = pl.ds(pl.multiple_of(j * tile, tile), tile)
            y = jnp.dot(hidden[rows], weight[j // per, :, inside], preferred_element_type=jnp.float32)
            parts[layer][rows, at] = y.astype(jnp.bfloat16)

    def enter(b):
        x = tokens[own_rows(b)].astype(jnp.float32)
        rows0[batch(b, t)] = rms_scale(x, early_norm[...]).astype(jnp.bfloat16)
        gather_send(0, b, 1)

    def middle(b):
        keep = (
            tokens[own_rows(b)].astype(jnp.float32)
            + 0.5 * rms_scale(sum_own(0, b), early_post[...])
            + rms_scale(mixer[own_rows(b)].astype(jnp.float32), mixer_gain[...])
        ).astype(jnp.bfloat16)
        mixed[own_rows(b)] = keep
        rows1[batch(b, t)] = rms_scale(keep.astype(jnp.float32), later_norm[...]).astype(jnp.bfloat16)
        gather_send(1, b, 1)

    def leave(b):
        out[own_rows(b)] = (
            mixed[own_rows(b)].astype(jnp.float32) + 0.5 * rms_scale(sum_own(1, b), later_post[...])
        ).astype(jnp.bfloat16)

    first, last = 0, U - 1
    start_weights(0)
    start_weights(1)
    enter(0)
    for m in range(2, 6):
        start_weights(m)
    for b in range(1, B):
        enter(b)
    for b in range(B):
        for d in range(1, T):
            if d == 2:
                relay(("y", b, first))
            gather_step(0, b, d)
    relay(("y", 2, first))
    relay(("x", 1, last))
    ready(0)
    ready(1)
    up(0, 0)
    relay(("y", 2, last))
    for b in range(1, B):
        up(0, b)
    relay(("x", 2, last))
    ready(2)
    for b in range(B):
        down(0, b)
        sum_first(0, b)
    for i in range(T - 1):
        sum_step(0, 0, i)
        relay(("x", 3, (first, last)[i > 0]))
    middle(0)
    for b in range(1, B):
        for i in range(T - 1):
            sum_step(0, b, i)
            gather_step(1, b - 1, i + 1)
            relay((("y", 4, last), ("x", 4, first), ("y", 5, first))[min(i, 2)])
        middle(b)
        if b == 1:
            relay(("x", 4, last))
            ready(3)
            ready(4)
        up(1, b - 1)
        if b == 1:
            relay(("y", 5, last))
            relay(("x", 5, last))
            ready(5)
        down(1, b - 1)
        sum_first(1, b - 1)
    for d in range(1, T):
        gather_step(1, B - 1, d)
    if B == 1:
        relay(("x", 5, last))
        for m in (3, 4, 5):
            ready(m)
    up(1, B - 1)
    down(1, B - 1)
    sum_first(1, B - 1)
    for b in range(B):
        for i in range(T - 1):
            sum_step(1, b, i)
        leave(b)
    for when, copy in sent:
        pl.when(when)(copy.wait_send)
    for copy in pending:
        copy.wait_send()


def on_device(sizes, *args):
    R, F, T = sizes
    (tokens, mixer, early_norm, eg, ev, ed, early_post, mixer_gain, later_norm, lg, lv, ld, later_post) = args
    n, D = tokens.shape
    depth, wide = eg.shape
    bf16 = jnp.bfloat16
    gains = [x.reshape(1, D) for x in (early_norm, early_post, mixer_gain, later_norm, later_post)]
    vmem = pl.BlockSpec(memory_space=pltpu.VMEM)
    hbm = pl.BlockSpec(memory_space=pl.ANY)
    gathered = [pltpu.VMEM((F * depth, wide), bf16)] * 2 + [pltpu.VMEM((F,) + ed.shape, bf16)]
    G = F // CORES
    U = max(1, 4 // G)
    B = 2
    w_count = 6 * (1 + U * (G - 1) * 2 * R)
    z_count = 8 * B * T
    return pl.pallas_call(
        functools.partial(kernel, R, F, T, B),
        out_shape=jax.ShapeDtypeStruct((n, D), bf16),
        in_specs=[vmem] * 3 + [hbm] * 3 + [vmem] * 3 + [hbm] * 3 + [vmem],
        out_specs=vmem,
        scratch_shapes=gathered * 2
        + [
            pltpu.VMEM((T * n, D), bf16),
            pltpu.VMEM((T * n, D), bf16),
            pltpu.VMEM((T * n, wide), bf16),
            pltpu.VMEM((T * n, D), bf16),
            pltpu.VMEM((T * n, D), bf16),
            pltpu.VMEM((n, D), bf16),
            pltpu.VMEM((2 * B * T, n // B, D), bf16),
            pltpu.VMEM((2 * B * T, n // B, D), bf16),
            pltpu.VMEM((n // B, D), jnp.float32),
            pltpu.SemaphoreType.DMA((w_count,)),
            pltpu.SemaphoreType.DMA((w_count,)),
            pltpu.SemaphoreType.DMA((6,)),
            pltpu.SemaphoreType.DMA((z_count,)),
            pltpu.SemaphoreType.DMA((z_count,)),
        ],
        compiler_params=pltpu.CompilerParams(
            collective_id=0, has_side_effects=True, vmem_limit_bytes=66_000_000
        ),
    )(tokens, mixer, gains[0], eg, ev, ed, gains[1], gains[2], gains[3], lg, lv, ld, gains[4])


def solution(mesh):
    placed = (
        P(("rep", "fs", "tp"), None),
        P(("rep", "fs", "tp"), None),
        P(),
        P("fs", "tp"),
        P("fs", "tp"),
        P("tp", "fs"),
        P(),
        P(),
        P(),
        P("fs", "tp"),
        P("fs", "tp"),
        P("tp", "fs"),
        P(),
    )
    sizes = tuple(mesh.shape[name] for name in ("rep", "fs", "tp"))
    return jax.shard_map(
        functools.partial(on_device, sizes),
        mesh=mesh,
        in_specs=placed,
        out_specs=P(("rep", "fs", "tp"), None),
        check_vma=False,
    )
```
